32 devices in a mesh: sp: 16 (over z, x, core), tp: 2 (over y).
Axes of the slice: x: 2, y: 2, z: 4, core: 2. Of those that a mesh axis runs over, the one named last changes fastest.
Arguments:
- moe_input: bfloat16 [2048, 2048], P('sp'), may hold values from -6 to 6
- out_cotangent: bfloat16 [2048, 2048], P('sp'), may hold values from -6 to 6
- routes: int32 [2048, 2], P('sp'), may hold values from 0 to 3, all different within a row; in each aligned block of 128 rows (0 to 127, 128 to 255, ...) at most 64 rows name the same one
- route_weight: float32 [2048, 2], P('sp'), may hold values from 0.2 to 1
- w_gate: bfloat16 [16, 2048, 896], P('sp', None, 'tp'), may hold values from -0.125 to 0.125
- w_up: bfloat16 [16, 2048, 896], P('sp', None, 'tp'), may hold values from -0.125 to 0.125
- w_down: bfloat16 [16, 896, 2048], P('sp', 'tp'), may hold values from -0.09375 to 0.09375
- out_proj: bfloat16 [2048, 1024], P(None, 'tp'), may hold values from -0.243067956 to 0.243067956
- conv_out: bfloat16 [2048, 1024], P('sp', 'tp'), may hold values from -17 to 17
- glu_value: bfloat16 [2048, 1024], P('sp', 'tp'), may hold values from -6 to 6
- glu_gate: bfloat16 [2048, 1024], P('sp', 'tp'), may hold values from -9 to 9
- taps: float32 [31, 1024], P(None, 'tp'), may hold values from -1 to 1
- norm_gain: float32 [1024], P('tp'), may hold values from 0.1 to 1.9
Outputs:
- grad_gate: bfloat16 [16, 2048, 896], P('sp', None, 'tp')
- grad_up: bfloat16 [16, 2048, 896], P('sp', None, 'tp')
- grad_down: bfloat16 [16, 896, 2048], P('sp', 'tp')
- grad_proj: float32 [2048, 1024], P('sp', 'tp')
- grad_glu_value: bfloat16 [2048, 1024], P('sp', 'tp')
- grad_glu_gate: bfloat16 [2048, 1024], P('sp', 'tp')
The draws below stay inside these ranges and needn't reach their ends.
Inputs may be any that keep to these rules, and one draw needn't show every extreme that they name: `routes`: each token names two different experts. Within the 128 tokens of one index of sp no expert is named more than 64 times, a bound that some block reaches.
All inputs are finite; a program needn't handle non-finite values.
Results may differ from the reference program's by a relative error of at most 0.014.
Values may be sent and summed in bfloat16 or wider, within the bound.
A program may use at most 128 MiB of HBM per device.

```python
import math
import jax
import jax.numpy as jnp
import numpy as np
from jax import lax

D = 2048
DB = 1024
FF = 3584
WIDTH = 31
SPAN = 4
TOK_DEV = 128
TOKENS = 2048
EXPERTS = 4
CAP = 64
N_SP = 16
N_TP = 2


def channel_profile(rough_key, lowest, highest):
    rising = jnp.exp(jnp.linspace(math.log(lowest), math.log(highest), DB)).astype(jnp.float32)
    rough = jnp.exp(jax.random.uniform(rough_key, (DB,), jnp.float32, -0.35, 0.35))
    return rising * rough


def draw_out_proj(key, part):
    base_key, rough_key = jax.random.split(jax.random.fold_in(key, 11), 2)
    profile = channel_profile(rough_key, 0.6, 1.8)
    values = jnp.clip(jax.random.normal(base_key, (D, DB), jnp.float32), -4.0, 4.0)
    return (values * profile[None, :] / math.sqrt(D)).astype(jnp.bfloat16)


def draw_conv_out(key, part):
    base_key, rough_key = jax.random.split(jax.random.fold_in(key, 23), 2)
    profile = channel_profile(rough_key, 0.5, 2.0)
    values = jnp.clip(jax.random.normal(base_key, (TOKENS, DB), jnp.float32), -4.0, 4.0)
    return (values * profile[None, :]).astype(jnp.bfloat16)


def raised(drawn, rng, source, target, shards_of, factor):
    def block_of(position):
        return (jnp.arange(drawn.shape[position]) // (drawn.shape[position] // shards_of)).reshape((-1,) + (1,) * (drawn.ndim - 1 - position))

    near = jax.random.permutation(rng, shards_of)[block_of(target)]
    other_side = (block_of(target) + shards_of // 2) % shards_of
    return jnp.where((block_of(source) == near) | (block_of(source) == other_side), factor * drawn, drawn)


def steps_of(key, shape, shards, low, top_value):
    gain, own = 1.0, jax.random.fold_in(key, 6)
    for position, parts in shards:
        draws = jnp.exp(jax.random.uniform(jax.random.fold_in(own, position), (parts,), jnp.float32, low / len(shards), top_value / len(shards)))
        gain = gain * jnp.repeat(draws, shape[position] // parts).reshape([-1 if axis == position else 1 for axis in range(len(shape))])
    return gain


def shared_out(key, own, number, rows, amount, top, reach, skew):
    sequence = jax.random.permutation(key, amount)
    heavy_load, common = portions_of(amount, rows * top, reach, skew, True), portions_of(amount, rows * top, reach, skew, False)
    places = jnp.arange(amount)

    def named(sizes, offset_by):
        used = int((sizes > 0).sum())
        fixed = max(1, used // 4)
        moved = fixed + (places - fixed + offset_by * (used - fixed)) % max(1, amount - fixed)
        return jnp.zeros((amount,), jnp.int32).at[sequence[jnp.where(places < fixed, places, moved)]].set(jnp.asarray(sizes, jnp.int32))

    sizes = jnp.where(number % 4 == 0, named(heavy_load, number // 4), named(common, number - number // 4 - 1))
    mixed = jax.random.permutation(jax.random.fold_in(own, 3), amount)
    donor, receiver = mixed[0:amount // 2 * 2:2], mixed[1:amount // 2 * 2:2]
    room = jnp.minimum(sizes[donor] - 1, reach - sizes[receiver]) // 2
    room = jnp.where((donor == sequence[0]) | (receiver == sequence[0]) | (sizes[receiver] == 0), 0, jnp.maximum(room, 0))
    moved = jax.random.randint(jax.random.fold_in(own, 4), (amount // 2,), 0, 1 << 20) % (room + 1)
    sizes = sizes.at[donor].add(-moved).at[receiver].add(moved)
    items = jnp.searchsorted(jnp.cumsum(sizes), jnp.arange(rows * top), side="right").astype(jnp.int32)
    listing = items.reshape(top, rows).T
    listing = listing[jax.random.permutation(jax.random.fold_in(own, 1), rows)]
    offset_by = jax.random.randint(jax.random.fold_in(own, 2), (rows, 1), 0, top)
    return jnp.take_along_axis(listing, (jnp.arange(top)[None, :] + offset_by) % top, axis=1)


def portions_of(count, total, most, slope, full):
    weights = [(1 << 20) // math.isqrt(standing ** slope) + 1 for standing in range(1, count + 1)]
    largest = most if full else min(most, max(-(-total // count), total * weights[0] // sum(weights)))
    least = 1 if total - largest >= count - 1 else 0
    holding, surplus = [largest] + [least] * (count - 1), total - largest - least * (count - 1)
    while surplus > 0:
        free = [i for i in range(1, count) if holding[i] < largest] or [i for i in range(1, count) if holding[i] < most]
        mass, remaining = sum([weights[i] for i in free]), surplus
        for i in free:
            extra = min(most - holding[i], max(1, remaining * weights[i] // mass), surplus)
            holding[i] = holding[i] + extra
            surplus = surplus - extra
    return np.array(holding)


def scatter_about(key, extent, scale, reach, shards=(), held_as=jnp.bfloat16):
    array = scale * jax.random.normal(key, extent, jnp.float32)
    if shards:
        array = array * steps_of(key, extent, shards, -0.22, 0.18)
    return jnp.clip(array, -reach, reach).astype(held_as)


def gaussian_with(own_key, extent, deviation, most, pieces, heavy, kind=jnp.bfloat16):
    result = deviation * jax.random.normal(own_key, extent, jnp.float32)
    if pieces:
        result = result * steps_of(own_key, extent, pieces, -0.22, 0.18)
    return jnp.clip(raised(result, jax.random.fold_in(own_key, 3), *heavy), -most, most).astype(kind)


def setup_inputs(seed: int = 0) -> dict:
    splits = jax.random.split(jax.random.key(seed), 14)
    moe_input = scatter_about(splits[0], (TOKENS, D), 1.0, 6.0, ((0, 16),))
    out_cotangent = gaussian_with(splits[1], (TOKENS, D), 1.0, 6.0, ((0, 16),), (0, 1, 16, 2.0))
    routes_keys = jax.random.split(jax.random.fold_in(splits[2], 1), TOKENS // TOK_DEV)
    routes_turns = jax.random.permutation(jax.random.fold_in(splits[2], 3), TOKENS // TOK_DEV)
    routes = jax.vmap(lambda own, number: shared_out(jax.random.fold_in(splits[2], 2), own, number, TOK_DEV, EXPERTS, 2, CAP, 0))(routes_keys, routes_turns).reshape((TOKENS, 2))
    route_weight = jnp.clip(0.2 + 0.8 * jax.random.uniform(splits[3], (TOKENS, 2), jnp.float32) ** steps_of(splits[3], (TOKENS, 2), ((0, 16),), -0.2, 0.2), 0.2, 1.0)
    w_gate = scatter_about(splits[4], (EXPERTS * SPAN, D, FF // SPAN), D ** -0.5, 0.125, ((0, 16), (2, 2)))
    w_up = scatter_about(splits[5], (EXPERTS * SPAN, D, FF // SPAN), D ** -0.5, 0.125, ((0, 16), (2, 2)))
    w_down = scatter_about(splits[6], (EXPERTS * SPAN, FF // SPAN, D), FF ** -0.5, 0.09375, ((0, 16), (1, 2)))
    out_proj = draw_out_proj(jax.random.fold_in(splits[13], 71), 0)
    conv_out = draw_conv_out(jax.random.fold_in(splits[13], 71), 0)
    glu_value = scatter_about(splits[9], (TOKENS, DB), 1.0, 6.0, ((0, 16), (1, 2)))
    glu_gate = scatter_about(splits[10], (TOKENS, DB), 1.5, 9.0, ((0, 16), (1, 2)))
    taps = scatter_about(splits[11], (WIDTH, DB), WIDTH ** -0.5, 1.0, ((1, 2),), jnp.float32)
    norm_gain = jnp.clip(1.0 + 0.18 * jax.random.normal(splits[12], (DB,), jnp.float32), 0.1, 1.9)
    return {"moe_input": moe_input, "out_cotangent": out_cotangent, "routes": routes, "route_weight": route_weight, "w_gate": w_gate, "w_up": w_up, "w_down": w_down, "out_proj": out_proj, "conv_out": conv_out, "glu_value": glu_value, "glu_gate": glu_gate, "taps": taps, "norm_gain": norm_gain}


def swish_slope(pre, sig):
    return sig * (1.0 + pre * (1.0 - sig))

def reference(moe_input, out_cotangent, routes, route_weight, w_gate, w_up, w_down, out_proj, conv_out, glu_value, glu_gate, taps, norm_gain):
    f32 = jnp.float32
    bf16 = jnp.bfloat16
    blocks = routes.reshape(N_SP, 2 * TOK_DEV)
    one_hot = (blocks[:, :, None] == jnp.arange(EXPERTS, dtype=jnp.int32)[None, None, :]).astype(jnp.int32)
    earlier = jnp.cumsum(one_hot, axis=1) - one_hot
    slot_index = lax.optimization_barrier(jnp.sum(earlier * one_hot, axis=2)).astype(jnp.int32)
    target = blocks * CAP + slot_index
    token_ids = jnp.arange(N_SP, dtype=jnp.int32)[:, None] * TOK_DEV + jnp.arange(2 * TOK_DEV, dtype=jnp.int32)[None, :] // 2
    matches = jnp.arange(EXPERTS * CAP, dtype=jnp.int32)[None, :, None] == target[:, None, :]
    source = lax.optimization_barrier(jnp.sum(jnp.where(matches, token_ids[:, None, :], 0), axis=2)).astype(jnp.int32)
    weights = lax.optimization_barrier(jnp.sum(jnp.where(matches, route_weight.reshape(N_SP, 1, 2 * TOK_DEV), 0.0), axis=2))
    filled = jnp.any(matches, axis=2)

    def by_expert(table):
        return jnp.transpose(table.reshape(N_SP, EXPERTS, CAP), (1, 0, 2)).reshape(EXPERTS, N_SP * CAP)
    ff_dev = FF // (SPAN * N_TP)
    contract_rows = (((0,), (0,)), ((), ()))

    def one_expert(inputs):
        expert, source_row, weight_row, filled_row = inputs
        expert_rows = jnp.where(filled_row[:, None], moe_input[source_row], jnp.zeros((), bf16))
        expert_cot = (weight_row[:, None] * out_cotangent[source_row].astype(f32)).astype(bf16)
        gate_w = jnp.transpose(lax.dynamic_slice_in_dim(w_gate, expert * SPAN, SPAN, 0), (1, 0, 2)).reshape(D, FF)
        up_w = jnp.transpose(lax.dynamic_slice_in_dim(w_up, expert * SPAN, SPAN, 0), (1, 0, 2)).reshape(D, FF)
        down_w = lax.dynamic_slice_in_dim(w_down, expert * SPAN, SPAN, 0).reshape(FF, D)
        gate_pre = jnp.dot(expert_rows, gate_w, preferred_element_type=f32)
        up_pre = jnp.dot(expert_rows, up_w, preferred_element_type=f32)
        gate_sig = jax.nn.sigmoid(gate_pre)
        hidden = (gate_pre * gate_sig * up_pre).astype(bf16)
        d_hidden = lax.dot_general(expert_cot, down_w, (((1,), (1,)), ((), ())), preferred_element_type=f32)
        grad_down = lax.dot_general(hidden, expert_cot, contract_rows, preferred_element_type=f32).astype(bf16)
        d_gate = (d_hidden * up_pre * swish_slope(gate_pre, gate_sig)).astype(bf16)
        d_up = (d_hidden * gate_pre * gate_sig).astype(bf16)
        grad_gate = lax.dot_general(expert_rows, d_gate, contract_rows, preferred_element_type=f32).astype(bf16)
        grad_up = lax.dot_general(expert_rows, d_up, contract_rows, preferred_element_type=f32).astype(bf16)
        row_count = expert_rows.shape[0]
        partial_value = jnp.einsum('rsjf,dsjf->sjrd', d_gate.reshape(row_count, SPAN, N_TP, ff_dev).astype(f32), gate_w.reshape(D, SPAN, N_TP, ff_dev).astype(f32))
        partial_value = partial_value + jnp.einsum('rsjf,dsjf->sjrd', d_up.reshape(row_count, SPAN, N_TP, ff_dev).astype(f32), up_w.reshape(D, SPAN, N_TP, ff_dev).astype(f32))
        partial_value = lax.optimization_barrier(partial_value.astype(bf16))
        span_part = lax.optimization_barrier(lax.optimization_barrier(jnp.sum(partial_value.astype(f32), axis=1)).astype(bf16))
        slot_grad = lax.optimization_barrier(jnp.sum(span_part.astype(f32), axis=0))
        gate_blocks = jnp.transpose(grad_gate.reshape(D, SPAN, FF // SPAN), (1, 0, 2))
        up_blocks = jnp.transpose(grad_up.reshape(D, SPAN, FF // SPAN), (1, 0, 2))
        down_blocks = grad_down.reshape(SPAN, FF // SPAN, D)
        return (gate_blocks, up_blocks, down_blocks, slot_grad)
    gate_all, up_all, down_all, slot_grads = lax.map(one_expert, (jnp.arange(EXPERTS, dtype=jnp.int32), by_expert(source), by_expert(weights), by_expert(filled)))
    grad_gate = gate_all.reshape(EXPERTS * SPAN, D, FF // SPAN)
    grad_up = up_all.reshape(EXPERTS * SPAN, D, FF // SPAN)
    grad_down = down_all.reshape(EXPERTS * SPAN, FF // SPAN, D)
    slot_table = slot_grads.reshape(EXPERTS, N_SP, CAP, D)
    per_route = slot_table[blocks, jnp.arange(N_SP, dtype=jnp.int32)[:, None], slot_index]
    moe_grad = lax.optimization_barrier(jnp.sum(per_route.reshape(TOKENS, 2, D), axis=1))
    resid_grad = (out_cotangent.astype(f32) + moe_grad).astype(bf16)
    conv_vals = conv_out.astype(f32)
    mean = lax.optimization_barrier(jnp.sum(conv_vals, axis=1, keepdims=True)) / DB
    square_mean = lax.optimization_barrier(jnp.sum(conv_vals * conv_vals, axis=1, keepdims=True)) / DB
    rstd = lax.rsqrt(square_mean - mean * mean + 1e-05)
    normed = (conv_vals - mean) * rstd
    zpre = normed * norm_gain[None, :]
    zsig = jax.nn.sigmoid(zpre)
    mixed = (zpre * zsig).astype(bf16)
    grad_proj = lax.dot_general(resid_grad, mixed, contract_rows, preferred_element_type=f32)
    d_mixed = jnp.dot(resid_grad, out_proj, preferred_element_type=f32)
    d_norm = d_mixed * swish_slope(zpre, zsig) * norm_gain[None, :]
    first_sum = lax.optimization_barrier(jnp.sum(d_norm, axis=1, keepdims=True)) / DB
    second_sum = lax.optimization_barrier(jnp.sum(d_norm * normed, axis=1, keepdims=True)) / DB
    conv_grad = (rstd * (d_norm - first_sum - normed * second_sum)).astype(bf16)
    extended = jnp.pad(conv_grad.astype(f32), ((0, WIDTH - 1), (0, 0)))
    unit_grad = lax.conv_general_dilated(extended[None], taps[:, None, :], (1,), 'VALID', dimension_numbers=('NWC', 'WIO', 'NWC'), feature_group_count=DB, precision=lax.Precision.HIGHEST)[0]
    gate_sig_in = jax.nn.sigmoid(glu_gate.astype(f32))
    grad_glu_value = (unit_grad * gate_sig_in).astype(bf16)
    grad_glu_gate = (unit_grad * glu_value.astype(f32) * gate_sig_in * (1.0 - gate_sig_in)).astype(bf16)
    return (grad_gate, grad_up, grad_down, grad_proj, grad_glu_value, grad_glu_gate)
```

```python
import functools

import jax
import jax.numpy as jnp
from jax import lax
from jax.experimental import pallas as pl
from jax.experimental.pallas import tpu as pltpu
from jax.sharding import PartitionSpec as P

F32 = jnp.float32
BF16 = jnp.bfloat16
ROWS = (((0,), (0,)), ((), ()))
UNITS = (((1,), (1,)), ((), ()))

DB = 1024
WIDTH = 31
SPAN = 4


def from_partner(array, axis, distance):
    return lax.ppermute(array, axis, [(i, i ^ 1 << distance) for i in range(lax.axis_size(axis))])


def from_behind(block, axis, distance):
    devices = range(lax.axis_size(axis))
    route = [(i - distance, i) for i in devices if i - distance in devices]
    return lax.ppermute(block, axis, route)


def swish_slope(pre, sig):
    return sig * (1.0 + pre * (1.0 - sig))


def route_places(routes, experts, capacity):
    flat_routes = routes.reshape(-1)
    one_hot = (flat_routes[:, None] == jnp.arange(experts, dtype=jnp.int32)[None, :]).astype(
        jnp.int32
    )
    earlier = jnp.cumsum(one_hot, axis=0) - one_hot
    slot_index = jnp.sum(earlier * one_hot, axis=1)
    return flat_routes * capacity + slot_index


def expert_pass(expert_rows, expert_cot, w_gate, w_up, w_down):
    gate_w = w_gate[0]
    up_w = w_up[0]
    down_w = w_down[0]
    contract_rows = (((0,), (0,)), ((), ()))
    contract_units = (((1,), (1,)), ((), ()))
    gate_pre = jnp.dot(expert_rows, gate_w, preferred_element_type=jnp.float32)
    up_pre = jnp.dot(expert_rows, up_w, preferred_element_type=jnp.float32)
    gate_sig = jax.nn.sigmoid(gate_pre)
    hidden = (gate_pre * gate_sig * up_pre).astype(jnp.bfloat16)
    d_hidden = lax.dot_general(
        expert_cot, down_w, contract_units, preferred_element_type=jnp.float32
    )
    grad_down = lax.dot_general(
        hidden, expert_cot, contract_rows, preferred_element_type=jnp.float32
    ).astype(jnp.bfloat16)
    d_gate = (d_hidden * up_pre * swish_slope(gate_pre, gate_sig)).astype(jnp.bfloat16)
    d_up = (d_hidden * gate_pre * gate_sig).astype(jnp.bfloat16)
    grad_gate = lax.dot_general(
        expert_rows, d_gate, contract_rows, preferred_element_type=jnp.float32
    ).astype(jnp.bfloat16)
    grad_up = lax.dot_general(
        expert_rows, d_up, contract_rows, preferred_element_type=jnp.float32
    ).astype(jnp.bfloat16)
    total = lax.dot_general(gate_w, d_gate, contract_units, preferred_element_type=jnp.float32)
    summed = lax.psum_scatter(
        (
            total + lax.dot_general(up_w, d_up, contract_units, preferred_element_type=jnp.float32)
        ).astype(jnp.bfloat16),
        "tp",
        scatter_dimension=0,
        tiled=True,
    )
    return (grad_gate[None], grad_up[None], grad_down[None], summed)


def local(
    moe_input,
    out_cotangent,
    routes,
    route_weight,
    w_gate,
    w_up,
    w_down,
    out_proj,
    conv_out,
    glu_value,
    glu_gate,
    taps,
    norm_gain,
):
    n_sp = lax.axis_size("sp")
    experts = n_sp // SPAN
    tok_rows = routes.shape[0]
    capacity = SPAN * min(tok_rows // SPAN, 2 * tok_rows // (experts * SPAN))
    sub_cap = capacity // SPAN
    model_width = moe_input.shape[1]
    span_bits = SPAN.bit_length() - 1
    my_index = lax.axis_index("sp")
    target = route_places(routes, experts, capacity)
    matches = jnp.arange(experts * capacity, dtype=jnp.int32)[:, None] == target[None, :]
    token_ids = jnp.arange(2 * tok_rows, dtype=jnp.int32) // 2
    source = jnp.sum(jnp.where(matches, token_ids[None, :], 0), axis=1)
    weights = jnp.sum(jnp.where(matches, route_weight.reshape(-1)[None, :], 0.0), axis=1)
    filled = jnp.any(matches, axis=1)
    send_rows = jnp.where(filled[:, None], moe_input[source], jnp.zeros((), jnp.bfloat16))
    send_cot = (weights[:, None] * out_cotangent[source].astype(jnp.float32)).astype(jnp.bfloat16)
    recv_rows, recv_cot = (
        lax.all_to_all(
            send_rows.reshape(n_sp, sub_cap, model_width),
            "sp",
            split_axis=0,
            concat_axis=0,
            tiled=True,
        ),
        lax.all_to_all(
            send_cot.reshape(n_sp, sub_cap, model_width),
            "sp",
            split_axis=0,
            concat_axis=0,
            tiled=True,
        ),
    )
    stacked = jnp.stack([recv_rows, recv_cot])[:, None]
    for bit_pos in range(span_bits):
        partner = from_partner(stacked, "sp", bit_pos)
        upper = my_index >> bit_pos & 1 == 1
        stacked = jnp.where(
            upper,
            jnp.concatenate([partner, stacked], axis=1),
            jnp.concatenate([stacked, partner], axis=1),
        )
    expert_rows = stacked[0].reshape(-1, model_width)
    expert_cot = stacked[1].reshape(-1, model_width)
    grad_gate, grad_up, grad_down, row_grads = expert_pass(
        expert_rows, expert_cot, w_gate, w_up, w_down
    )
    part_width = row_grads.shape[0]
    partial_sums = row_grads.reshape(part_width, SPAN, n_sp, sub_cap)
    for section, bit_pos in enumerate(reversed(range(span_bits))):
        half = partial_sums.shape[1] // 2
        upper = my_index >> bit_pos & 1 == 1
        lower_half = partial_sums[:, :half]
        upper_half = partial_sums[:, half:]
        kept = jnp.where(upper, upper_half, lower_half)
        sent = jnp.where(upper, lower_half, upper_half)
        if section == 0:
            arrived = from_partner(sent, "sp", bit_pos)
            partial_sums = kept.astype(jnp.float32) + arrived.astype(jnp.float32)
        else:
            partial_sums = kept + from_partner(sent, "sp", bit_pos)
    returned = lax.all_to_all(partial_sums, "sp", split_axis=2, concat_axis=2, tiled=True)
    slot_grads = returned.reshape(part_width, experts * capacity)
    per_route = jnp.take(slot_grads, target, axis=1).reshape(part_width, tok_rows, 2)
    moe_grad = jnp.sum(per_route, axis=2)
    own_cot = lax.dynamic_slice_in_dim(
        out_cotangent, lax.axis_index("tp") * part_width, part_width, 1
    )
    resid_part = (own_cot.astype(jnp.float32).T + moe_grad).astype(jnp.bfloat16)
    resid_grad = lax.all_gather(resid_part, "tp", axis=0, tiled=True)
    conv_vals = conv_out.astype(jnp.float32)
    total_sum, square_sum = lax.psum(
        (jnp.sum(conv_vals, axis=1), jnp.sum(conv_vals * conv_vals, axis=1)), "tp"
    )
    mean = total_sum[:, None] / DB
    rstd = lax.rsqrt(square_sum[:, None] / DB - mean * mean + 1e-05)
    normed = (conv_vals - mean) * rstd
    zpre = normed * norm_gain[None, :]
    zsig = jax.nn.sigmoid(zpre)
    mixed = (zpre * zsig).astype(jnp.bfloat16)
    grad_proj = lax.psum_scatter(
        jnp.dot(resid_grad, mixed, preferred_element_type=jnp.float32),
        "sp",
        scatter_dimension=0,
        tiled=True,
    )
    d_mixed = lax.dot_general(
        resid_grad, out_proj, (((0,), (0,)), ((), ())), preferred_element_type=jnp.float32
    )
    d_norm = d_mixed * swish_slope(zpre, zsig) * norm_gain[None, :]
    first_sum, second_sum = lax.psum(
        (jnp.sum(d_norm, axis=1), jnp.sum(d_norm * normed, axis=1)), "tp"
    )
    conv_grad = (
        rstd * (d_norm - first_sum[:, None] / DB - normed * second_sum[:, None] / DB)
    ).astype(jnp.bfloat16)
    later_rows = from_behind(conv_grad[: WIDTH - 1], "sp", -1)
    extended = jnp.concatenate([conv_grad, later_rows], axis=0).astype(jnp.float32)
    unit_grad = lax.conv_general_dilated(
        extended[None],
        taps[:, None, :],
        (1,),
        "VALID",
        dimension_numbers=("NWC", "WIO", "NWC"),
        feature_group_count=taps.shape[1],
        precision=lax.Precision.HIGHEST,
    )[0]
    gate_sig_in = jax.nn.sigmoid(glu_gate.astype(jnp.float32))
    grad_glu_value = (unit_grad * gate_sig_in).astype(jnp.bfloat16)
    grad_glu_gate = (
        unit_grad * glu_value.astype(jnp.float32) * gate_sig_in * (1.0 - gate_sig_in)
    ).astype(jnp.bfloat16)
    return (grad_gate, grad_up, grad_down, grad_proj, grad_glu_value, grad_glu_gate)


def send(src, dst, send_sem, recv_sem, sp, tp):
    return pltpu.make_async_remote_copy(
        src_ref=src,
        dst_ref=dst,
        send_sem=send_sem,
        recv_sem=recv_sem,
        device_id={"sp": sp, "tp": tp},
        device_id_type=pl.DeviceIdType.MESH,
    )


def greet(peers):
    barrier = pltpu.get_barrier_semaphore()
    for sp, tp in peers:
        pl.semaphore_signal(
            barrier, inc=1, device_id={"sp": sp, "tp": tp}, device_id_type=pl.DeviceIdType.MESH
        )
    return lambda: pl.semaphore_wait(barrier, len(peers))


def near_first(groups):
    order = [0]
    for step in range(1, groups // 2 + 1):
        order += [step] if step == groups - step else [step, groups - step]
    return order if groups > 1 else [0]


def place():
    s, t = lax.axis_index("sp"), lax.axis_index("tp")
    q, r = s // SPAN, s % SPAN
    x, c = r // 2, r % 2
    rx = 2 * (1 - x) + c
    rc = 2 * x + 1 - c
    rxc = 2 * (1 - x) + 1 - c
    return s, t, 1 - t, q, r, x, c, rx, rc, rxc


def dispatch_kernel(
    groups, x_ref, g_ref, routes_ref, weight_ref, conv_ref, gain_ref,
    xo, mo, pt_ref, stat_ref,
    sb, xs, ms, st, st_in,
    z_s, z_r, x_s, x_r, y_s, y_r, a_s, a_r, b_s, b_r, c_s, c_r,
    mz_s, mz_r, mx_s, mx_r, mc_s, mc_r, st_s, st_r, o_s, mo_s,
):
    s, t, u, q, r, _, _, rx, rc, rxc = place()
    n_sp = groups * SPAN
    tok, width = x_ref.shape
    cap = sb.shape[2]
    half = width // 2
    mine = pl.ds(pl.multiple_of(t * half, 128), half)
    other = pl.ds(pl.multiple_of(u * half, 128), half)
    order = near_first(groups)
    at_x, at_c, at_y = (q * SPAN + rx, t), (q * SPAN + rc, t), (s, u)
    peers = [(lax.rem(q + d, groups) * SPAN + r, t) for d in order[1:]]
    ready = greet(peers + [at_x, at_c, at_y])

    lane = lax.broadcasted_iota(jnp.int32, (tok, 128), 1)
    hot = [(routes_ref[:, k : k + 1] == lane).astype(F32) for k in range(2)]
    before = (
        lax.broadcasted_iota(jnp.int32, (tok, tok), 1) < lax.broadcasted_iota(jnp.int32, (tok, tok), 0)
    ).astype(BF16)
    counts = jnp.dot(before, (hot[0] + hot[1]).astype(BF16), preferred_element_type=F32)
    spots = lax.broadcasted_iota(jnp.int32, (tok, groups * cap), 1)
    pts, cots = [], []
    for k in range(2):
        slot = jnp.sum(counts * hot[k], axis=1, keepdims=True).astype(jnp.int32)
        target = routes_ref[:, k : k + 1] * cap + slot
        pts.append((target == spots).astype(F32).astype(BF16))
    pt = pts[0] + pts[1]
    pt_ref[...] = pt
    chunk = 512
    for j in range(0, width, chunk):
        cols = slice(j, j + chunk)
        rows = lax.dot_general(pt, x_ref[:, cols], ROWS, preferred_element_type=F32)
        sb[0, :, :, cols] = rows.astype(BF16).reshape(groups, cap, chunk)
        cot = g_ref[:, cols].astype(F32)
        total = None
        for k in range(2):
            part = lax.dot_general(
                pts[k],
                (weight_ref[:, k : k + 1] * cot).astype(BF16),
                ROWS,
                preferred_element_type=F32,
            )
            total = part if total is None else total + part
        sb[1, :, :, cols] = total.astype(BF16).reshape(groups, cap, chunk)
    conv = conv_ref[...].astype(F32)
    first = jnp.sum(conv, axis=1, keepdims=True)
    second = jnp.sum(conv * conv, axis=1, keepdims=True)
    st[...] = jnp.where(lane == 0, first, second)
    ready()

    started = []

    def go(copy):
        copy.start()
        started.append(copy)

    for d in order[1:]:
        to = lax.rem(q + d, groups)
        go(send(sb.at[:, to, :, mine], xs.at[:, s, :, mine], z_s.at[d], z_r.at[d], to * SPAN + r, t))
    go(send(st, st_in, st_s, st_r, *at_y))

    def stage_one(d):
        b = lax.rem(q - d + groups, groups) * SPAN + r
        dst = xs.at[:, b, :, mine]
        if d:
            send(dst, dst, z_s.at[d], z_r.at[d], s, t).wait_recv()
        src = dst if d else sb.at[:, q, :, mine]
        go(send(src, dst, x_s.at[d], x_r.at[d], *at_x))
        go(send(src, dst, y_s.at[d], y_r.at[d], *at_y))
        go(send(src, dst, c_s.at[d, 0], c_r.at[d, 0], *at_c))

    def diag_a(d):
        return pl.ds(0, 2) if d == 0 else pl.ds(0, 1)

    def stage_two(d):
        base = lax.rem(q - d + groups, groups) * SPAN
        got = xs.at[:, base + rx, :, mine]
        send(got, got, x_s.at[d], x_r.at[d], *at_x).wait_recv()
        part = xs.at[diag_a(d), base + rx, :, mine]
        go(send(part, part, a_s.at[d], a_r.at[d], *at_y))
        go(send(got, got, c_s.at[d, 1], c_r.at[d, 1], *at_c))
        got = xs.at[:, base + r, :, other]
        send(got, got, y_s.at[d], y_r.at[d], *at_y).wait_recv()
        if d:
            part = xs.at[pl.ds(1, 1), base + r, :, other]
            go(send(part, part, b_s.at[d], b_r.at[d], *at_x))
        go(send(got, got, c_s.at[d, 2], c_r.at[d, 2], *at_c))

    def stage_three(d):
        b = lax.rem(q - d + groups, groups) * SPAN + rx
        part = xs.at[diag_a(d), b, :, other]
        send(part, part, a_s.at[d], a_r.at[d], *at_y).wait_recv()
        if d:
            part = xs.at[pl.ds(1, 1), b, :, other]
            send(part, part, b_s.at[d], b_r.at[d], *at_x).wait_recv()
        got = xs.at[:, b, :, other]
        go(send(got, got, c_s.at[d, 3], c_r.at[d, 3], *at_c))

    def finish(d):
        base = lax.rem(q - d + groups, groups) * SPAN
        for i, (place_in, cols) in enumerate([(rc, mine), (rxc, mine), (rc, other), (rxc, other)]):
            got = xs.at[:, base + place_in, :, cols]
            send(got, got, c_s.at[d, i], c_r.at[d, i], *at_c).wait_recv()
        span = pl.ds(base, SPAN)
        out = pltpu.make_async_copy(xs.at[:, span], xo.at[:, span], o_s.at[d])
        out.start()
        return out

    stage_one(0)
    xs[:, s, :, mine] = sb[:, q, :, mine]
    send(st, st_in, st_s, st_r, *at_y).wait_recv()
    sums = st[...] + st_in[...]
    channels = conv_ref.shape[1] * 2
    mean = sums[:, 0:1] / channels
    rstd = lax.rsqrt(sums[:, 1:2] / channels - mean * mean + 1e-05)
    stat_ref[...] = jnp.where(lane == 0, mean, rstd)
    zpre = (conv - mean) * rstd * gain_ref[...]
    ms[s] = (zpre * jax.nn.sigmoid(zpre)).astype(BF16)
    for d in order[1:]:
        to = lax.rem(q + d, groups)
        go(send(ms.at[s], ms.at[s], mz_s.at[d], mz_r.at[d], to * SPAN + r, t))

    outs = []
    for i in range(groups + 2):
        if 0 < i < groups:
            stage_one(order[i])
        if 0 < i <= groups:
            stage_two(order[i - 1])
        if i > 1:
            stage_three(order[i - 2])
            d = order[i - 2]
            got = ms.at[lax.rem(q - d + groups, groups) * SPAN + r]
            if d:
                send(got, got, mz_s.at[d], mz_r.at[d], s, t).wait_recv()
            go(send(got, got, mx_s.at[d], mx_r.at[d], *at_x))
            go(send(got, got, mc_s.at[d, 0], mc_r.at[d, 0], *at_c))
    for d in order:
        outs.append(finish(d))
    for d in order:
        got = ms.at[lax.rem(q - d + groups, groups) * SPAN + rx]
        send(got, got, mx_s.at[d], mx_r.at[d], *at_x).wait_recv()
        go(send(got, got, mc_s.at[d, 1], mc_r.at[d, 1], *at_c))
    for d in order:
        base = lax.rem(q - d + groups, groups) * SPAN
        for i, place_in in enumerate([rc, rxc]):
            got = ms.at[base + place_in]
            send(got, got, mc_s.at[d, i], mc_r.at[d, i], *at_c).wait_recv()
    out = pltpu.make_async_copy(ms, mo, mo_s)
    out.start()
    outs.append(out)
    for copy in started:
        copy.wait_send()
    for copy in outs:
        copy.wait()


def combine_kernel(
    groups, t_ref, pt_ref, stat_ref, g_ref, proj_ref, conv_ref, gain_ref, value_ref, gate_ref, taps_ref, m_ref,
    gp_ref, gv_ref, gg_ref,
    core_in, s1, rx1, ry1, sa, sbb, rx2, ry2, fin, rz, rt, rr, st, st_in, ext, halo, halo_in, slope_ref, normed_ref,
    c_s, c_r, x1_s, x1_r, y1_s, y1_r, x2_s, x2_r, y2_s, y2_r, z_s, z_r,
    h_s, h_r, k_s, k_r, st_s, st_r, halo_s, halo_r,
):
    s, t, u, q, r, x, c, rx, rc, _ = place()
    xb, cb = 1 - x, 1 - c
    n_sp = groups * SPAN
    tok, width = g_ref.shape
    cap = t_ref.shape[1]
    half = width // 2
    piece = half // 2
    block = width // n_sp
    order = near_first(groups)[::-1]
    at_x, at_c, at_y = (q * SPAN + rx, t), (q * SPAN + rc, t), (s, u)
    ready = greet([(lax.rem(s + d, n_sp), t) for d in range(1, n_sp)] + [at_y])
    lane = lax.broadcasted_iota(jnp.int32, (tok, 128), 1)
    started = []

    def go(copy):
        copy.start()
        started.append(copy)

    def recv(dst, recv_sem):
        send(dst, dst, recv_sem, recv_sem, *at_y).wait_recv()

    def add(a, b):
        return (a.astype(F32) + b.astype(F32)).astype(BF16)

    ready()
    for d in order:
        to = lax.rem(q + d, groups)
        for i in range(2):
            go(send(t_ref.at[to * SPAN + 2 * i + cb], core_in.at[d, i], c_s.at[d, i], c_r.at[d, i], *at_c))

    def stage_one(d):
        to = lax.rem(q + d, groups)
        for i in range(2):
            recv(core_in.at[d, i], c_r.at[d, i])
            for h in range(2):
                for p in range(2):
                    cols = slice(h * half + p * piece, h * half + (p + 1) * piece)
                    s1[d, i, p, h] = add(t_ref[to * SPAN + 2 * i + c, :, cols], core_in[d, i, :, cols])
        go(send(s1.at[d, xb, 0], rx1.at[d], x1_s.at[d], x1_r.at[d], *at_x))
        go(send(s1.at[d, :, 1, u], ry1.at[d], y1_s.at[d], y1_r.at[d], *at_y))

    def stage_two(d):
        recv(rx1.at[d], x1_r.at[d])
        for h in range(2):
            sa[d, h] = add(s1[d, x, 0, h], rx1[d, h])
        go(send(sa.at[d, u], ry2.at[d], y2_s.at[d], y2_r.at[d], *at_y))
        recv(ry1.at[d], y1_r.at[d])
        for i in range(2):
            sbb[d, i] = add(s1[d, i, 1, t], ry1[d, i])
        go(send(sbb.at[d, xb], rx2.at[d], x2_s.at[d], x2_r.at[d], *at_x))

    def stage_three(d):
        recv(ry2.at[d], y2_r.at[d])
        low = add(sa[d, t], ry2[d])
        recv(rx2.at[d], x2_r.at[d])
        high = add(sbb[d, x], rx2[d])
        if d:
            fin[d, :, :piece] = low
            fin[d, :, piece:] = high
            to = lax.rem(q + d, groups) * SPAN + r
            go(send(fin.at[d], rz.at[q], z_s.at[d], z_r.at[d], to, t))
        else:
            rz[q, :, :piece] = low
            rz[q, :, piece:] = high

    for i in range(groups + 2):
        if i < groups:
            stage_one(order[i])
        if i == 1:
            normed = (conv_ref[...].astype(F32) - stat_ref[:, 0:1]) * stat_ref[:, 1:2]
            zpre = normed * gain_ref[...]
            sig = jax.nn.sigmoid(zpre)
            normed_ref[...] = normed
            slope_ref[...] = swish_slope(zpre, sig) * gain_ref[...]
        if 0 < i <= groups:
            stage_two(order[i - 1])
        if i > 1:
            stage_three(order[i - 2])
    for d in order:
        if d:
            recv(rz.at[lax.rem(q - d + groups, groups)], z_r.at[d])

    eye = (
        lax.broadcasted_iota(jnp.int32, (tok, tok), 0) == lax.broadcasted_iota(jnp.int32, (tok, tok), 1)
    ).astype(F32).astype(BF16)
    pt = pt_ref[...]
    chunk = 256
    for j in range(0, half, chunk):
        own = g_ref[:, pl.ds(pl.multiple_of(t * half + j, 128), chunk)]
        slots = rz[:, :, j : j + chunk].reshape(groups * cap, chunk)
        total = lax.dot_general(own, eye, ROWS, preferred_element_type=F32) + lax.dot_general(
            slots, pt, (((0,), (1,)), ((), ())), preferred_element_type=F32
        )
        rt[pl.ds(pl.multiple_of(t * half + j, 128), chunk), :] = total.astype(BF16)
    mine = rt.at[pl.ds(pl.multiple_of(t * half, 128), half)]
    other = rt.at[pl.ds(pl.multiple_of(u * half, 128), half)]
    go(send(mine, mine, h_s, h_r, *at_y))

    def rows_of(to):
        return rt.at[pl.ds(pl.multiple_of(to * block, block), block)]

    def column_of(source):
        return rr.at[:, pl.ds(pl.multiple_of(source * tok, 128), tok)]

    def scatter(part):
        for d in range(n_sp // 2):
            to = part * (n_sp // 2) + lax.rem(s + d, n_sp // 2)

            @pl.when(to != s)
            def _():
                send(rows_of(to), column_of(s), k_s.at[to], k_r.at[s], to, t).start()

    scatter(t)
    recv(other, h_r)
    scatter(u)
    rr[:, pl.ds(pl.multiple_of(s * tok, 128), tok)] = rt[pl.ds(pl.multiple_of(s * block, block), block), :]

    d_mixed = lax.dot_general(rt[...], proj_ref[...], ROWS, preferred_element_type=F32)
    channels = 2 * conv_ref.shape[1]
    d_norm = d_mixed * slope_ref[...]
    normed = normed_ref[...]
    first = jnp.sum(d_norm, axis=1, keepdims=True)
    second = jnp.sum(d_norm * normed, axis=1, keepdims=True)
    st[...] = jnp.where(lane == 0, first, second)
    go(send(st, st_in, st_s, st_r, *at_y))
    recv(st_in, st_r)
    sums = st[...] + st_in[...]
    conv_grad = stat_ref[:, 1:2] * (
        d_norm - sums[:, 0:1] / channels - normed * (sums[:, 1:2] / channels)
    )
    conv_grad = conv_grad.astype(BF16)
    reach = halo.shape[0]
    halo[...] = conv_grad[:reach]

    @pl.when(s > 0)
    def _():
        send(halo, halo_in, halo_s, halo_r, s - 1, t).start()

    ext[:tok] = conv_grad.astype(F32)
    halo_in_needed = s < n_sp - 1

    @pl.when(halo_in_needed)
    def _():
        recv(halo_in, halo_r)
        ext[tok:] = halo_in[...].astype(F32)

    @pl.when(jnp.logical_not(halo_in_needed))
    def _():
        ext[tok:] = jnp.zeros((reach, ext.shape[1]), F32)

    lanes = 128
    for j in range(0, ext.shape[1], lanes):
        cols = slice(j, j + lanes)
        total = taps_ref[0:1, cols] * ext[0:tok, cols]
        for k in range(1, taps_ref.shape[0]):
            total = total + taps_ref[k : k + 1, cols] * ext[k : k + tok, cols]
        sig = jax.nn.sigmoid(gate_ref[:, cols].astype(F32))
        gv_ref[:, cols] = (total * sig).astype(BF16)
        gg_ref[:, cols] = (total * value_ref[:, cols].astype(F32) * sig * (1.0 - sig)).astype(BF16)

    for d in range(1, n_sp):
        source = lax.rem(s + n_sp - d, n_sp)
        recv(column_of(source), k_r.at[source])
    gp_ref[...] = jnp.dot(
        rr[...], m_ref[...].reshape(n_sp * tok, m_ref.shape[2]), preferred_element_type=F32
    )
    for copy in started:
        copy.wait_send()

    @pl.when(s > 0)
    def _():
        send(halo, halo_in, halo_s, halo_r, s - 1, t).wait_send()

    for d in range(1, n_sp):
        to = lax.rem(s + d, n_sp)
        send(rows_of(to), column_of(s), k_s.at[to], k_r.at[s], to, t).wait_send()


def paired(
    moe_input, out_cotangent, routes, route_weight, w_gate, w_up, w_down, out_proj, conv_out, glu_value, glu_gate, taps, norm_gain
):
    n_sp = lax.axis_size("sp")
    groups = n_sp // SPAN
    tok, width = moe_input.shape
    channels = conv_out.shape[1]
    cap = SPAN * min(tok // SPAN, 2 * tok // (groups * SPAN))
    vmem = pl.BlockSpec(memory_space=pltpu.VMEM)
    hbm = pl.BlockSpec(memory_space=pl.ANY)
    dma = pltpu.SemaphoreType.DMA
    gain = norm_gain[None]
    rows, mixed_all, pt, stat = pl.pallas_call(
        functools.partial(dispatch_kernel, groups),
        out_shape=(
            jax.ShapeDtypeStruct((2, n_sp, cap, width), BF16),
            jax.ShapeDtypeStruct((n_sp, tok, channels), BF16),
            jax.ShapeDtypeStruct((tok, groups * cap), BF16),
            jax.ShapeDtypeStruct((tok, 128), F32),
        ),
        in_specs=[vmem] * 6,
        out_specs=(hbm, hbm, vmem, vmem),
        scratch_shapes=[
            pltpu.VMEM((2, groups, cap, width), BF16),
            pltpu.VMEM((2, n_sp, cap, width), BF16),
            pltpu.VMEM((n_sp, tok, channels), BF16),
            pltpu.VMEM((tok, 128), F32),
            pltpu.VMEM((tok, 128), F32),
        ]
        + [dma((groups,))] * 10
        + [dma((groups, 4))] * 2
        + [dma((groups,))] * 4
        + [dma((groups, 2))] * 2
        + [dma] * 2
        + [dma((groups,)), dma],
        compiler_params=pltpu.CompilerParams(
            collective_id=0, has_side_effects=True, vmem_limit_bytes=36 << 20
        ),
        name="dispatch",
    )(moe_input, out_cotangent, routes, route_weight, conv_out, gain)
    expert_rows = rows[0].reshape(n_sp * cap, width)
    expert_cot = rows[1].reshape(n_sp * cap, width)
    grad_gate, grad_up, grad_down, part = expert_products(expert_rows, expert_cot, w_gate, w_up, w_down)
    reach = -(-(WIDTH - 1) // 16) * 16
    half = width // 2
    piece = half // 2
    pair = pltpu.VMEM((groups, 2, cap, piece), BF16)
    single = pltpu.VMEM((groups, cap, piece), BF16)
    grad_proj, grad_value, grad_gate_in = pl.pallas_call(
        functools.partial(combine_kernel, groups),
        out_shape=(
            jax.ShapeDtypeStruct((width // n_sp, channels), F32),
            jax.ShapeDtypeStruct((tok, channels), BF16),
            jax.ShapeDtypeStruct((tok, channels), BF16),
        ),
        in_specs=[vmem] * 11,
        out_specs=(vmem,) * 3,
        scratch_shapes=[
            pltpu.VMEM((groups, 2, cap, width), BF16),
            pltpu.VMEM((groups, 2, 2, 2, cap, piece), BF16),
            pair, pair, pair, pair, single, single,
            pltpu.VMEM((groups, cap, half), BF16),
            pltpu.VMEM((groups, cap, half), BF16),
            pltpu.VMEM((width, tok), BF16),
            pltpu.VMEM((width // n_sp, n_sp * tok), BF16),
            pltpu.VMEM((tok, 128), F32),
            pltpu.VMEM((tok, 128), F32),
            pltpu.VMEM((tok + reach, channels), F32),
            pltpu.VMEM((reach, channels), BF16),
            pltpu.VMEM((reach, channels), BF16),
            pltpu.VMEM((tok, channels), F32),
            pltpu.VMEM((tok, channels), F32),
        ]
        + [dma((groups, 2))] * 2
        + [dma((groups,))] * 10
        + [dma] * 2
        + [dma((n_sp,))] * 2
        + [dma] * 4,
        compiler_params=pltpu.CompilerParams(
            collective_id=1, has_side_effects=True, vmem_limit_bytes=48 << 20
        ),
        name="combine",
    )(
        part.reshape(n_sp, cap, width),
        pt, stat, out_cotangent, out_proj, conv_out, gain, glu_value, glu_gate, taps, mixed_all,
    )
    return (grad_gate, grad_up, grad_down, grad_proj, grad_value, grad_gate_in)


def expert_products(expert_rows, expert_cot, w_gate, w_up, w_down):
    gate_w, up_w, down_w = w_gate[0], w_up[0], w_down[0]
    gate_pre = jnp.dot(expert_rows, gate_w, preferred_element_type=F32)
    up_pre = jnp.dot(expert_rows, up_w, preferred_element_type=F32)
    gate_sig = jax.nn.sigmoid(gate_pre)
    hidden = (gate_pre * gate_sig * up_pre).astype(BF16)
    d_hidden = lax.dot_general(expert_cot, down_w, UNITS, preferred_element_type=F32)
    grad_down = lax.dot_general(hidden, expert_cot, ROWS, preferred_element_type=F32).astype(BF16)
    d_gate = (d_hidden * up_pre * swish_slope(gate_pre, gate_sig)).astype(BF16)
    d_up = (d_hidden * gate_pre * gate_sig).astype(BF16)
    grad_gate = lax.dot_general(expert_rows, d_gate, ROWS, preferred_element_type=F32).astype(BF16)
    grad_up = lax.dot_general(expert_rows, d_up, ROWS, preferred_element_type=F32).astype(BF16)
    part = (
        lax.dot_general(d_gate, gate_w, UNITS, preferred_element_type=F32)
        + lax.dot_general(d_up, up_w, UNITS, preferred_element_type=F32)
    ).astype(BF16)
    return grad_gate[None], grad_up[None], grad_down[None], part


def solution(mesh):
    in_specs = (
        P("sp", None),
        P("sp", None),
        P("sp", None),
        P("sp", None),
        P("sp", None, "tp"),
        P("sp", None, "tp"),
        P("sp", "tp", None),
        P(None, "tp"),
        P("sp", "tp"),
        P("sp", "tp"),
        P("sp", "tp"),
        P(None, "tp"),
        P("tp"),
    )
    out_specs = (
        P("sp", None, "tp"),
        P("sp", None, "tp"),
        P("sp", "tp", None),
        P("sp", "tp"),
        P("sp", "tp"),
        P("sp", "tp"),
    )
    body = paired if mesh.shape["tp"] == 2 else local
    return jax.shard_map(body, mesh=mesh, in_specs=in_specs, out_specs=out_specs, check_vma=False)
```

```python
import functools

import jax
import jax.numpy as jnp
from jax import lax
from jax.experimental import pallas as pl
from jax.experimental.pallas import tpu as pltpu
from jax.sharding import PartitionSpec as P

F32 = jnp.float32
BF16 = jnp.bfloat16
ROWS = (((0,), (0,)), ((), ()))
UNITS = (((1,), (1,)), ((), ()))

DB = 1024
WIDTH = 31
SPAN = 4


def from_partner(array, axis, distance):
    return lax.ppermute(array, axis, [(i, i ^ 1 << distance) for i in range(lax.axis_size(axis))])


def from_behind(block, axis, distance):
    devices = range(lax.axis_size(axis))
    route = [(i - distance, i) for i in devices if i - distance in devices]
    return lax.ppermute(block, axis, route)


def swish_slope(pre, sig):
    return sig * (1.0 + pre * (1.0 - sig))


def route_places(routes, experts, capacity):
    flat_routes = routes.reshape(-1)
    one_hot = (flat_routes[:, None] == jnp.arange(experts, dtype=jnp.int32)[None, :]).astype(
        jnp.int32
    )
    earlier = jnp.cumsum(one_hot, axis=0) - one_hot
    slot_index = jnp.sum(earlier * one_hot, axis=1)
    return flat_routes * capacity + slot_index


def expert_pass(expert_rows, expert_cot, w_gate, w_up, w_down):
    gate_w = w_gate[0]
    up_w = w_up[0]
    down_w = w_down[0]
    contract_rows = (((0,), (0,)), ((), ()))
    contract_units = (((1,), (1,)), ((), ()))
    gate_pre = jnp.dot(expert_rows, gate_w, preferred_element_type=jnp.float32)
    up_pre = jnp.dot(expert_rows, up_w, preferred_element_type=jnp.float32)
    gate_sig = jax.nn.sigmoid(gate_pre)
    hidden = (gate_pre * gate_sig * up_pre).astype(jnp.bfloat16)
    d_hidden = lax.dot_general(
        expert_cot, down_w, contract_units, preferred_element_type=jnp.float32
    )
    grad_down = lax.dot_general(
        hidden, expert_cot, contract_rows, preferred_element_type=jnp.float32
    ).astype(jnp.bfloat16)
    d_gate = (d_hidden * up_pre * swish_slope(gate_pre, gate_sig)).astype(jnp.bfloat16)
    d_up = (d_hidden * gate_pre * gate_sig).astype(jnp.bfloat16)
    grad_gate = lax.dot_general(
        expert_rows, d_gate, contract_rows, preferred_element_type=jnp.float32
    ).astype(jnp.bfloat16)
    grad_up = lax.dot_general(
        expert_rows, d_up, contract_rows, preferred_element_type=jnp.float32
    ).astype(jnp.bfloat16)
    total = lax.dot_general(gate_w, d_gate, contract_units, preferred_element_type=jnp.float32)
    summed = lax.psum_scatter(
        (
            total + lax.dot_general(up_w, d_up, contract_units, preferred_element_type=jnp.float32)
        ).astype(jnp.bfloat16),
        "tp",
        scatter_dimension=0,
        tiled=True,
    )
    return (grad_gate[None], grad_up[None], grad_down[None], summed)


def local(
    moe_input,
    out_cotangent,
    routes,
    route_weight,
    w_gate,
    w_up,
    w_down,
    out_proj,
    conv_out,
    glu_value,
    glu_gate,
    taps,
    norm_gain,
):
    n_sp = lax.axis_size("sp")
    experts = n_sp // SPAN
    tok_rows = routes.shape[0]
    capacity = SPAN * min(tok_rows // SPAN, 2 * tok_rows // (experts * SPAN))
    sub_cap = capacity // SPAN
    model_width = moe_input.shape[1]
    span_bits = SPAN.bit_length() - 1
    my_index = lax.axis_index("sp")
    target = route_places(routes, experts, capacity)
    matches = jnp.arange(experts * capacity, dtype=jnp.int32)[:, None] == target[None, :]
    token_ids = jnp.arange(2 * tok_rows, dtype=jnp.int32) // 2
    source = jnp.sum(jnp.where(matches, token_ids[None, :], 0), axis=1)
    weights = jnp.sum(jnp.where(matches, route_weight.reshape(-1)[None, :], 0.0), axis=1)
    filled = jnp.any(matches, axis=1)
    send_rows = jnp.where(filled[:, None], moe_input[source], jnp.zeros((), jnp.bfloat16))
    send_cot = (weights[:, None] * out_cotangent[source].astype(jnp.float32)).astype(jnp.bfloat16)
    recv_rows, recv_cot = (
        lax.all_to_all(
            send_rows.reshape(n_sp, sub_cap, model_width),
            "sp",
            split_axis=0,
            concat_axis=0,
            tiled=True,
        ),
        lax.all_to_all(
            send_cot.reshape(n_sp, sub_cap, model_width),
            "sp",
            split_axis=0,
            concat_axis=0,
            tiled=True,
        ),
    )
    stacked = jnp.stack([recv_rows, recv_cot])[:, None]
    for bit_pos in range(span_bits):
        partner = from_partner(stacked, "sp", bit_pos)
        upper = my_index >> bit_pos & 1 == 1
        stacked = jnp.where(
            upper,
            jnp.concatenate([partner, stacked], axis=1),
            jnp.concatenate([stacked, partner], axis=1),
        )
    expert_rows = stacked[0].reshape(-1, model_width)
    expert_cot = stacked[1].reshape(-1, model_width)
    grad_gate, grad_up, grad_down, row_grads = expert_pass(
        expert_rows, expert_cot, w_gate, w_up, w_down
    )
    part_width = row_grads.shape[0]
    partial_sums = row_grads.reshape(part_width, SPAN, n_sp, sub_cap)
    for section, bit_pos in enumerate(reversed(range(span_bits))):
        half = partial_sums.shape[1] // 2
        upper = my_index >> bit_pos & 1 == 1
        lower_half = partial_sums[:, :half]
        upper_half = partial_sums[:, half:]
        kept = jnp.where(upper, upper_half, lower_half)
        sent = jnp.where(upper, lower_half, upper_half)
        if section == 0:
            arrived = from_partner(sent, "sp", bit_pos)
            partial_sums = kept.astype(jnp.float32) + arrived.astype(jnp.float32)
        else:
            partial_sums = kept + from_partner(sent, "sp", bit_pos)
    returned = lax.all_to_all(partial_sums, "sp", split_axis=2, concat_axis=2, tiled=True)
    slot_grads = returned.reshape(part_width, experts * capacity)
    per_route = jnp.take(slot_grads, target, axis=1).reshape(part_width, tok_rows, 2)
    moe_grad = jnp.sum(per_route, axis=2)
    own_cot = lax.dynamic_slice_in_dim(
        out_cotangent, lax.axis_index("tp") * part_width, part_width, 1
    )
    resid_part = (own_cot.astype(jnp.float32).T + moe_grad).astype(jnp.bfloat16)
    resid_grad = lax.all_gather(resid_part, "tp", axis=0, tiled=True)
    conv_vals = conv_out.astype(jnp.float32)
    total_sum, square_sum = lax.psum(
        (jnp.sum(conv_vals, axis=1), jnp.sum(conv_vals * conv_vals, axis=1)), "tp"
    )
    mean = total_sum[:, None] / DB
    rstd = lax.rsqrt(square_sum[:, None] / DB - mean * mean + 1e-05)
    normed = (conv_vals - mean) * rstd
    zpre = normed * norm_gain[None, :]
    zsig = jax.nn.sigmoid(zpre)
    mixed = (zpre * zsig).astype(jnp.bfloat16)
    grad_proj = lax.psum_scatter(
        jnp.dot(resid_grad, mixed, preferred_element_type=jnp.float32),
        "sp",
        scatter_dimension=0,
        tiled=True,
    )
    d_mixed = lax.dot_general(
        resid_grad, out_proj, (((0,), (0,)), ((), ())), preferred_element_type=jnp.float32
    )
    d_norm = d_mixed * swish_slope(zpre, zsig) * norm_gain[None, :]
    first_sum, second_sum = lax.psum(
        (jnp.sum(d_norm, axis=1), jnp.sum(d_norm * normed, axis=1)), "tp"
    )
    conv_grad = (
        rstd * (d_norm - first_sum[:, None] / DB - normed * second_sum[:, None] / DB)
    ).astype(jnp.bfloat16)
    later_rows = from_behind(conv_grad[: WIDTH - 1], "sp", -1)
    extended = jnp.concatenate([conv_grad, later_rows], axis=0).astype(jnp.float32)
    unit_grad = lax.conv_general_dilated(
        extended[None],
        taps[:, None, :],
        (1,),
        "VALID",
        dimension_numbers=("NWC", "WIO", "NWC"),
        feature_group_count=taps.shape[1],
        precision=lax.Precision.HIGHEST,
    )[0]
    gate_sig_in = jax.nn.sigmoid(glu_gate.astype(jnp.float32))
    grad_glu_value = (unit_grad * gate_sig_in).astype(jnp.bfloat16)
    grad_glu_gate = (
        unit_grad * glu_value.astype(jnp.float32) * gate_sig_in * (1.0 - gate_sig_in)
    ).astype(jnp.bfloat16)
    return (grad_gate, grad_up, grad_down, grad_proj, grad_glu_value, grad_glu_gate)


def send(src, dst, send_sem, recv_sem, sp, tp):
    return pltpu.make_async_remote_copy(
        src_ref=src,
        dst_ref=dst,
        send_sem=send_sem,
        recv_sem=recv_sem,
        device_id={"sp": sp, "tp": tp},
        device_id_type=pl.DeviceIdType.MESH,
    )


def greet(peers):
    barrier = pltpu.get_barrier_semaphore()
    for sp, tp in peers:
        pl.semaphore_signal(
            barrier, inc=1, device_id={"sp": sp, "tp": tp}, device_id_type=pl.DeviceIdType.MESH
        )
    return lambda: pl.semaphore_wait(barrier, len(peers))


def near_first(groups):
    order = [0]
    for step in range(1, groups // 2 + 1):
        order += [step] if step == groups - step else [step, groups - step]
    return order if groups > 1 else [0]


def place():
    s, t = lax.axis_index("sp"), lax.axis_index("tp")
    q, r = s // SPAN, s % SPAN
    x, c = r // 2, r % 2
    rx = 2 * (1 - x) + c
    rc = 2 * x + 1 - c
    rxc = 2 * (1 - x) + 1 - c
    return s, t, 1 - t, q, r, x, c, rx, rc, rxc


def dispatch_kernel(
    groups, x_hbm, g_hbm, routes_ref, weight_ref, conv_hbm, gain_ref, gw_hbm, uw_hbm, dw_hbm,
    xo, co, mo, pt_ref, stat_ref, hid_ref, dg_ref, du_ref,
    x_ref, g_ref, conv_ref, gw, uw, dw, sb, xs, ms, st, st_in,
    z_s, z_r, x_s, x_r, y_s, y_r, a_s, a_r, b_s, b_r, c_s, c_r,
    mz_s, mz_r, mx_s, mx_r, mc_s, mc_r, st_s, st_r, o_s, mo_s, w_s,
):
    s, t, u, q, r, _, _, rx, rc, rxc = place()
    tok, width = x_ref.shape
    cap = sb.shape[2]
    half = width // 2
    mine = pl.ds(pl.multiple_of(t * half, 128), half)
    other = pl.ds(pl.multiple_of(u * half, 128), half)
    order = near_first(groups)
    at_x, at_c, at_y = (q * SPAN + rx, t), (q * SPAN + rc, t), (s, u)
    peers = [(lax.rem(q + d, groups) * SPAN + r, t) for d in order[1:]]
    ready = greet(peers + [at_x, at_c, at_y])

    pairs = [(x_hbm, x_ref), (g_hbm, g_ref), (conv_hbm, conv_ref), (gw_hbm, gw), (uw_hbm, uw), (dw_hbm, dw)]
    loads = [
        pltpu.make_async_copy(src, dst, w_s.at[i])
        for i, (src, dst) in enumerate(pairs)
    ]
    for copy in loads:
        copy.start()

    lane = lax.broadcasted_iota(jnp.int32, (tok, 128), 1)
    eye = lane == lax.broadcasted_iota(jnp.int32, (tok, tok), 0)

    def column(row):
        return jnp.sum(jnp.where(eye, row, jnp.zeros_like(row)), axis=1, keepdims=True)

    routes = [column(routes_ref[k : k + 1, :].astype(F32)).astype(jnp.int32) for k in range(2)]
    weights = [column(weight_ref[k : k + 1, :]) for k in range(2)]
    hot = [(routes[k] == lane).astype(F32) for k in range(2)]
    before = (
        lax.broadcasted_iota(jnp.int32, (tok, tok), 1) < lax.broadcasted_iota(jnp.int32, (tok, tok), 0)
    ).astype(BF16)
    counts = jnp.dot(before, (hot[0] + hot[1]).astype(BF16), preferred_element_type=F32)
    spots = lax.broadcasted_iota(jnp.int32, (tok, groups * cap), 1)
    pts, cots = [], []
    for k in range(2):
        slot = jnp.sum(counts * hot[k], axis=1, keepdims=True).astype(jnp.int32)
        target = routes[k] * cap + slot
        pts.append((target == spots).astype(F32).astype(BF16))
    pt = pts[0] + pts[1]
    pt_ref[...] = pt
    chunk = 512
    for copy in loads[:3]:
        copy.wait()
    for j in range(0, width, chunk):
        cols = slice(j, j + chunk)
        rows = lax.dot_general(pt, x_ref[:, cols], ROWS, preferred_element_type=F32)
        sb[0, :, :, cols] = rows.astype(BF16).reshape(groups, cap, chunk)
        cot = g_ref[:, cols].astype(F32)
        total = None
        for k in range(2):
            part = lax.dot_general(
                pts[k],
                (weights[k] * cot).astype(BF16),
                ROWS,
                preferred_element_type=F32,
            )
            total = part if total is None else total + part
        sb[1, :, :, cols] = total.astype(BF16).reshape(groups, cap, chunk)
    conv = conv_ref[...].astype(F32)
    first = jnp.sum(conv, axis=1, keepdims=True)
    second = jnp.sum(conv * conv, axis=1, keepdims=True)
    st[...] = jnp.where(lane == 0, first, second)
    ready()

    started, outs = [], []

    def go(copy):
        copy.start()
        started.append(copy)

    for d in order[1:]:
        to = lax.rem(q + d, groups)
        go(send(sb.at[:, to, :, mine], xs.at[:, s, :, mine], z_s.at[d], z_r.at[d], to * SPAN + r, t))
    go(send(st, st_in, st_s, st_r, *at_y))

    def stage_one(d):
        b = lax.rem(q - d + groups, groups) * SPAN + r
        dst = xs.at[:, b, :, mine]
        if d:
            send(dst, dst, z_s.at[d], z_r.at[d], s, t).wait_recv()
        src = dst if d else sb.at[:, q, :, mine]
        go(send(src, dst, x_s.at[d], x_r.at[d], *at_x))
        go(send(src, dst, y_s.at[d], y_r.at[d], *at_y))
        go(send(src, dst, c_s.at[d, 0], c_r.at[d, 0], *at_c))

    def diag_a(d):
        return pl.ds(0, 2) if d == 0 else pl.ds(0, 1)

    def stage_two(d):
        base = lax.rem(q - d + groups, groups) * SPAN
        got = xs.at[:, base + rx, :, mine]
        send(got, got, x_s.at[d], x_r.at[d], *at_x).wait_recv()
        part = xs.at[diag_a(d), base + rx, :, mine]
        go(send(part, part, a_s.at[d], a_r.at[d], *at_y))
        go(send(got, got, c_s.at[d, 1], c_r.at[d, 1], *at_c))
        got = xs.at[:, base + r, :, other]
        send(got, got, y_s.at[d], y_r.at[d], *at_y).wait_recv()
        if d:
            part = xs.at[pl.ds(1, 1), base + r, :, other]
            go(send(part, part, b_s.at[d], b_r.at[d], *at_x))
        go(send(got, got, c_s.at[d, 2], c_r.at[d, 2], *at_c))

    def stage_three(d):
        b = lax.rem(q - d + groups, groups) * SPAN + rx
        part = xs.at[diag_a(d), b, :, other]
        send(part, part, a_s.at[d], a_r.at[d], *at_y).wait_recv()
        if d:
            part = xs.at[pl.ds(1, 1), b, :, other]
            send(part, part, b_s.at[d], b_r.at[d], *at_x).wait_recv()
        got = xs.at[:, b, :, other]
        go(send(got, got, c_s.at[d, 3], c_r.at[d, 3], *at_c))

    def finish(d):
        base = lax.rem(q - d + groups, groups) * SPAN
        for i, (place_in, cols) in enumerate([(rc, mine), (rxc, mine), (rc, other), (rxc, other)]):
            got = xs.at[:, base + place_in, :, cols]
            send(got, got, c_s.at[d, i], c_r.at[d, i], *at_c).wait_recv()
        span = pl.ds(base, SPAN)
        for i, dst in enumerate([xo, co]):
            out = pltpu.make_async_copy(xs.at[i, span], dst.at[span], o_s.at[d, i])
            out.start()
            outs.append(out)
        if d == 0:
            for copy in loads[3:]:
                copy.wait()
        rows = xs[0, span].reshape(SPAN * cap, width)
        cot = xs[1, span].reshape(SPAN * cap, width)
        gate_pre = lax.dot_general(rows, gw[...], UNITS, preferred_element_type=F32)
        up_pre = lax.dot_general(rows, uw[...], UNITS, preferred_element_type=F32)
        d_hidden = lax.dot_general(cot, dw[...], UNITS, preferred_element_type=F32)
        sig = jax.nn.sigmoid(gate_pre)
        silu = gate_pre * sig
        into = pl.ds(pl.multiple_of(base * cap, SPAN * cap), SPAN * cap)
        hid_ref[into, :] = (silu * up_pre).astype(BF16)
        dg_ref[into, :] = (d_hidden * up_pre * swish_slope(gate_pre, sig)).astype(BF16)
        du_ref[into, :] = (d_hidden * silu).astype(BF16)

    stage_one(0)
    xs[:, s, :, mine] = sb[:, q, :, mine]
    send(st, st_in, st_s, st_r, *at_y).wait_recv()
    sums = st[...] + st_in[...]
    channels = conv_ref.shape[1] * 2
    mean = sums[:, 0:1] / channels
    rstd = lax.rsqrt(sums[:, 1:2] / channels - mean * mean + 1e-05)
    stat_ref[...] = jnp.where(lane == 0, mean, rstd)
    zpre = (conv - mean) * rstd * gain_ref[...]
    ms[s] = (zpre * jax.nn.sigmoid(zpre)).astype(BF16)
    for d in order[1:]:
        to = lax.rem(q + d, groups)
        go(send(ms.at[s], ms.at[s], mz_s.at[d], mz_r.at[d], to * SPAN + r, t))

    for i in range(groups + 2):
        if 0 < i < groups:
            stage_one(order[i])
        if 0 < i <= groups:
            stage_two(order[i - 1])
        if i > 1:
            stage_three(order[i - 2])
            d = order[i - 2]
            got = ms.at[lax.rem(q - d + groups, groups) * SPAN + r]
            if d:
                send(got, got, mz_s.at[d], mz_r.at[d], s, t).wait_recv()
            go(send(got, got, mx_s.at[d], mx_r.at[d], *at_x))
            go(send(got, got, mc_s.at[d, 0], mc_r.at[d, 0], *at_c))
        if i > 2:
            finish(order[i - 3])
    for d in order:
        got = ms.at[lax.rem(q - d + groups, groups) * SPAN + rx]
        send(got, got, mx_s.at[d], mx_r.at[d], *at_x).wait_recv()
        go(send(got, got, mc_s.at[d, 1], mc_r.at[d, 1], *at_c))
    finish(order[-1])
    for d in order:
        base = lax.rem(q - d + groups, groups) * SPAN
        for i, place_in in enumerate([rc, rxc]):
            got = ms.at[base + place_in]
            send(got, got, mc_s.at[d, i], mc_r.at[d, i], *at_c).wait_recv()
    out = pltpu.make_async_copy(ms, mo, mo_s)
    out.start()
    outs.append(out)
    for copy in started:
        copy.wait_send()
    for copy in outs:
        copy.wait()


def combine_kernel(
    groups, dg_ref, du_ref, gw_ref, uw_ref, pt_ref, stat_ref, g_ref, proj_ref, conv_ref, gain_ref, value_ref, gate_ref, taps_ref, m_ref,
    gp_ref, gv_ref, gg_ref,
    t_ref, core_in, s1, rx1, ry1, sa, sbb, rx2, ry2, fin, rz, rt, rr, st, st_in, ext, halo, halo_in, slope_ref, normed_ref,
    c_s, c_r, x1_s, x1_r, y1_s, y1_r, x2_s, x2_r, y2_s, y2_r, z_s, z_r,
    h_s, h_r, k_s, k_r, st_s, st_r, halo_s, halo_r,
):
    s, t, u, q, r, x, c, rx, rc, _ = place()
    xb, cb = 1 - x, 1 - c
    n_sp = groups * SPAN
    tok, width = g_ref.shape
    cap = t_ref.shape[1]
    half = width // 2
    piece = half // 2
    block = width // n_sp
    order = near_first(groups)[::-1]
    at_x, at_c, at_y = (q * SPAN + rx, t), (q * SPAN + rc, t), (s, u)
    ready = greet([(lax.rem(s + d, n_sp), t) for d in range(1, n_sp)] + [at_y])
    lane = lax.broadcasted_iota(jnp.int32, (tok, 128), 1)
    started = []

    def go(copy):
        copy.start()
        started.append(copy)

    def recv(dst, recv_sem):
        send(dst, dst, recv_sem, recv_sem, *at_y).wait_recv()

    def add(a, b):
        return (a.astype(F32) + b.astype(F32)).astype(BF16)

    ready()

    def products(d):
        to = lax.rem(q + d, groups)
        rows = pl.ds(pl.multiple_of(to * (SPAN * cap), SPAN * cap), SPAN * cap)
        chunk = 512
        for j in range(0, width, chunk):
            cols = slice(j, j + chunk)
            part = jnp.dot(dg_ref[rows, :], gw_ref[:, cols], preferred_element_type=F32)
            part = part + jnp.dot(du_ref[rows, :], uw_ref[:, cols], preferred_element_type=F32)
            t_ref[pl.ds(to * SPAN, SPAN), :, cols] = part.astype(BF16).reshape(SPAN, cap, chunk)
        for i in range(2):
            go(send(t_ref.at[to * SPAN + 2 * i + cb], core_in.at[d, i], c_s.at[d, i], c_r.at[d, i], *at_c))

    def stage_one(d):
        to = lax.rem(q + d, groups)
        for i in range(2):
            recv(core_in.at[d, i], c_r.at[d, i])
            for h in range(2):
                for p in range(2):
                    cols = slice(h * half + p * piece, h * half + (p + 1) * piece)
                    s1[d, i, p, h] = add(t_ref[to * SPAN + 2 * i + c, :, cols], core_in[d, i, :, cols])
        go(send(s1.at[d, xb, 0], rx1.at[d], x1_s.at[d], x1_r.at[d], *at_x))
        go(send(s1.at[d, :, 1, u], ry1.at[d], y1_s.at[d], y1_r.at[d], *at_y))

    def stage_two(d):
        recv(rx1.at[d], x1_r.at[d])
        for h in range(2):
            sa[d, h] = add(s1[d, x, 0, h], rx1[d, h])
        go(send(sa.at[d, u], ry2.at[d], y2_s.at[d], y2_r.at[d], *at_y))
        recv(ry1.at[d], y1_r.at[d])
        for i in range(2):
            sbb[d, i] = add(s1[d, i, 1, t], ry1[d, i])
        go(send(sbb.at[d, xb], rx2.at[d], x2_s.at[d], x2_r.at[d], *at_x))

    def stage_three(d):
        recv(ry2.at[d], y2_r.at[d])
        low = add(sa[d, t], ry2[d])
        recv(rx2.at[d], x2_r.at[d])
        high = add(sbb[d, x], rx2[d])
        if d:
            fin[d, :, :piece] = low
            fin[d, :, piece:] = high
            to = lax.rem(q + d, groups) * SPAN + r
            go(send(fin.at[d], rz.at[q], z_s.at[d], z_r.at[d], to, t))
        else:
            rz[q, :, :piece] = low
            rz[q, :, piece:] = high

    products(order[0])
    for i in range(groups + 2):
        if i + 1 < groups:
            products(order[i + 1])
        if i < groups:
            stage_one(order[i])
        if i == 1:
            normed = (conv_ref[...].astype(F32) - stat_ref[:, 0:1]) * stat_ref[:, 1:2]
            zpre = normed * gain_ref[...]
            sig = jax.nn.sigmoid(zpre)
            normed_ref[...] = normed
            slope_ref[...] = swish_slope(zpre, sig) * gain_ref[...]
        if 0 < i <= groups:
            stage_two(order[i - 1])
        if i > 1:
            stage_three(order[i - 2])
    for d in order:
        if d:
            recv(rz.at[lax.rem(q - d + groups, groups)], z_r.at[d])

    eye = (
        lax.broadcasted_iota(jnp.int32, (tok, tok), 0) == lax.broadcasted_iota(jnp.int32, (tok, tok), 1)
    ).astype(F32).astype(BF16)
    pt = pt_ref[...]
    chunk = 256
    for j in range(0, half, chunk):
        own = g_ref[:, pl.ds(pl.multiple_of(t * half + j, 128), chunk)]
        slots = rz[:, :, j : j + chunk].reshape(groups * cap, chunk)
        total = lax.dot_general(own, eye, ROWS, preferred_element_type=F32) + lax.dot_general(
            slots, pt, (((0,), (1,)), ((), ())), preferred_element_type=F32
        )
        rt[pl.ds(pl.multiple_of(t * half + j, 128), chunk), :] = total.astype(BF16)
    mine = rt.at[pl.ds(pl.multiple_of(t * half, 128), half)]
    other = rt.at[pl.ds(pl.multiple_of(u * half, 128), half)]
    go(send(mine, mine, h_s, h_r, *at_y))

    def rows_of(to):
        return rt.at[pl.ds(pl.multiple_of(to * block, block), block)]

    def column_of(source):
        return rr.at[:, pl.ds(pl.multiple_of(source * tok, 128), tok)]

    def scatter(part):
        for d in range(n_sp // 2):
            to = part * (n_sp // 2) + lax.rem(s + d, n_sp // 2)

            @pl.when(to != s)
            def _():
                send(rows_of(to), column_of(s), k_s.at[to], k_r.at[s], to, t).start()

    scatter(t)
    recv(other, h_r)
    scatter(u)
    rr[:, pl.ds(pl.multiple_of(s * tok, 128), tok)] = rt[pl.ds(pl.multiple_of(s * block, block), block), :]

    d_mixed = lax.dot_general(rt[...], proj_ref[...], ROWS, preferred_element_type=F32)
    channels = 2 * conv_ref.shape[1]
    d_norm = d_mixed * slope_ref[...]
    normed = normed_ref[...]
    first = jnp.sum(d_norm, axis=1, keepdims=True)
    second = jnp.sum(d_norm * normed, axis=1, keepdims=True)
    st[...] = jnp.where(lane == 0, first, second)
    go(send(st, st_in, st_s, st_r, *at_y))
    recv(st_in, st_r)
    sums = st[...] + st_in[...]
    conv_grad = stat_ref[:, 1:2] * (
        d_norm - sums[:, 0:1] / channels - normed * (sums[:, 1:2] / channels)
    )
    conv_grad = conv_grad.astype(BF16)
    reach = halo.shape[0]
    halo[...] = conv_grad[:reach]

    @pl.when(s > 0)
    def _():
        send(halo, halo_in, halo_s, halo_r, s - 1, t).start()

    ext[:tok] = conv_grad.astype(F32)
    halo_in_needed = s < n_sp - 1

    @pl.when(halo_in_needed)
    def _():
        recv(halo_in, halo_r)
        ext[tok:] = halo_in[...].astype(F32)

    @pl.when(jnp.logical_not(halo_in_needed))
    def _():
        ext[tok:] = jnp.zeros((reach, ext.shape[1]), F32)

    lanes = 128
    for j in range(0, ext.shape[1], lanes):
        cols = slice(j, j + lanes)
        total = taps_ref[0:1, cols] * ext[0:tok, cols]
        for k in range(1, taps_ref.shape[0]):
            total = total + taps_ref[k : k + 1, cols] * ext[k : k + tok, cols]
        sig = jax.nn.sigmoid(gate_ref[:, cols].astype(F32))
        gv_ref[:, cols] = (total * sig).astype(BF16)
        gg_ref[:, cols] = (total * value_ref[:, cols].astype(F32) * sig * (1.0 - sig)).astype(BF16)

    for d in range(1, n_sp):
        source = lax.rem(s + n_sp - d, n_sp)
        recv(column_of(source), k_r.at[source])
    gp_ref[...] = jnp.dot(
        rr[...], m_ref[...].reshape(n_sp * tok, m_ref.shape[2]), preferred_element_type=F32
    )
    for copy in started:
        copy.wait_send()

    @pl.when(s > 0)
    def _():
        send(halo, halo_in, halo_s, halo_r, s - 1, t).wait_send()

    for d in range(1, n_sp):
        to = lax.rem(s + d, n_sp)
        send(rows_of(to), column_of(s), k_s.at[to], k_r.at[s], to, t).wait_send()


def paired(
    moe_input, out_cotangent, routes, route_weight, w_gate, w_up, w_down, out_proj, conv_out, glu_value, glu_gate, taps, norm_gain
):
    n_sp = lax.axis_size("sp")
    groups = n_sp // SPAN
    tok, width = moe_input.shape
    channels = conv_out.shape[1]
    cap = SPAN * min(tok // SPAN, 2 * tok // (groups * SPAN))
    vmem = pl.BlockSpec(memory_space=pltpu.VMEM)
    hbm = pl.BlockSpec(memory_space=pl.ANY)
    pinned = pl.BlockSpec(memory_space=pltpu.MemorySpace.HBM)
    dma = pltpu.SemaphoreType.DMA
    gain = norm_gain[None]
    gate_w, up_w = jnp.swapaxes(w_gate[0], 0, 1), jnp.swapaxes(w_up[0], 0, 1)
    down_w = w_down[0]
    units = down_w.shape[0]
    unit_rows = jax.ShapeDtypeStruct((n_sp * cap, units), BF16)
    expert_rows, expert_cot, mixed_all, pt, stat, hidden, d_gate, d_up = pl.pallas_call(
        functools.partial(dispatch_kernel, groups),
        out_shape=(
            jax.ShapeDtypeStruct((n_sp, cap, width), BF16),
            jax.ShapeDtypeStruct((n_sp, cap, width), BF16),
            jax.ShapeDtypeStruct((n_sp, tok, channels), BF16),
            jax.ShapeDtypeStruct((tok, groups * cap), BF16),
            jax.ShapeDtypeStruct((tok, 128), F32),
            unit_rows,
            unit_rows,
            unit_rows,
        ),
        in_specs=[pinned, pinned, vmem, vmem, pinned, vmem] + [pinned] * 3,
        out_specs=(hbm,) * 3 + (vmem,) * 5,
        scratch_shapes=[
            pltpu.VMEM((tok, width), BF16),
            pltpu.VMEM((tok, width), BF16),
            pltpu.VMEM((tok, channels), BF16),
        ]
        + [pltpu.VMEM((units, width), BF16)] * 3
        + [
            pltpu.VMEM((2, groups, cap, width), BF16),
            pltpu.VMEM((2, n_sp, cap, width), BF16),
            pltpu.VMEM((n_sp, tok, channels), BF16),
            pltpu.VMEM((tok, 128), F32),
            pltpu.VMEM((tok, 128), F32),
        ]
        + [dma((groups,))] * 10
        + [dma((groups, 4))] * 2
        + [dma((groups,))] * 4
        + [dma((groups, 2))] * 2
        + [dma] * 2
        + [dma((groups, 2)), dma, dma((6,))],
        compiler_params=pltpu.CompilerParams(
            collective_id=0, has_side_effects=True, vmem_limit_bytes=63 << 20
        ),
        name="dispatch",
    )(moe_input, out_cotangent, routes.T, route_weight.T, conv_out, gain, gate_w, up_w, down_w)
    expert_rows = expert_rows.reshape(n_sp * cap, width)
    expert_cot = expert_cot.reshape(n_sp * cap, width)
    grad_down = lax.dot_general(hidden, expert_cot, ROWS, preferred_element_type=F32).astype(BF16)
    grad_gate = lax.dot_general(expert_rows, d_gate, ROWS, preferred_element_type=F32).astype(BF16)
    grad_up = lax.dot_general(expert_rows, d_up, ROWS, preferred_element_type=F32).astype(BF16)
    grad_gate, grad_up, grad_down, d_gate, d_up = lax.optimization_barrier(
        (grad_gate, grad_up, grad_down, d_gate, d_up)
    )
    reach = -(-(WIDTH - 1) // 16) * 16
    half = width // 2
    piece = half // 2
    pair = pltpu.VMEM((groups, 2, cap, piece), BF16)
    single = pltpu.VMEM((groups, cap, piece), BF16)
    grad_proj, grad_value, grad_gate_in = pl.pallas_call(
        functools.partial(combine_kernel, groups),
        out_shape=(
            jax.ShapeDtypeStruct((width // n_sp, channels), F32),
            jax.ShapeDtypeStruct((tok, channels), BF16),
            jax.ShapeDtypeStruct((tok, channels), BF16),
        ),
        in_specs=[vmem] * 14,
        out_specs=(vmem,) * 3,
        scratch_shapes=[
            pltpu.VMEM((n_sp, cap, width), BF16),
            pltpu.VMEM((groups, 2, cap, width), BF16),
            pltpu.VMEM((groups, 2, 2, 2, cap, piece), BF16),
            pair, pair, pair, pair, single, single,
            pltpu.VMEM((groups, cap, half), BF16),
            pltpu.VMEM((groups, cap, half), BF16),
            pltpu.VMEM((width, tok), BF16),
            pltpu.VMEM((width // n_sp, n_sp * tok), BF16),
            pltpu.VMEM((tok, 128), F32),
            pltpu.VMEM((tok, 128), F32),
            pltpu.VMEM((tok + reach, channels), F32),
            pltpu.VMEM((reach, channels), BF16),
            pltpu.VMEM((reach, channels), BF16),
            pltpu.VMEM((tok, channels), F32),
            pltpu.VMEM((tok, channels), F32),
        ]
        + [dma((groups, 2))] * 2
        + [dma((groups,))] * 10
        + [dma] * 2
        + [dma((n_sp,))] * 2
        + [dma] * 4,
        compiler_params=pltpu.CompilerParams(
            collective_id=1, has_side_effects=True, vmem_limit_bytes=48 << 20
        ),
        name="combine",
    )(
        d_gate, d_up, gate_w, up_w,
        pt, stat, out_cotangent, out_proj, conv_out, gain, glu_value, glu_gate, taps, mixed_all,
    )
    return (grad_gate[None], grad_up[None], grad_down[None], grad_proj, grad_value, grad_gate_in)


def solution(mesh):
    in_specs = (
        P("sp", None),
        P("sp", None),
        P("sp", None),
        P("sp", None),
        P("sp", None, "tp"),
        P("sp", None, "tp"),
        P("sp", "tp", None),
        P(None, "tp"),
        P("sp", "tp"),
        P("sp", "tp"),
        P("sp", "tp"),
        P(None, "tp"),
        P("tp"),
    )
    out_specs = (
        P("sp", None, "tp"),
        P("sp", None, "tp"),
        P("sp", "tp", None),
        P("sp", "tp"),
        P("sp", "tp"),
        P("sp", "tp"),
    )
    body = paired if mesh.shape["tp"] == 2 else local
    return jax.shard_map(body, mesh=mesh, in_specs=in_specs, out_specs=out_specs, check_vma=False)
```
